32 devices in a mesh: sp: 8 (over z, x), tp: 4 (over y, core).
Axes of the slice: x: 2, y: 2, z: 4, core: 2. Of those that a mesh axis runs over, the one named last changes fastest.
Arguments:
- conv_value: bfloat16 [4096, 1024], P('sp', 'tp'), may hold values from -6 to 6
- conv_gate: bfloat16 [4096, 1024], P('sp', 'tp'), may hold values from -9 to 9
- conv_weight: float32 [31, 1024], P(None, 'tp'), may hold values from -2.2 to 2.2
- conv_gain: float32 [1024], P('tp'), may hold values from 0.1 to 1.9
- conv_shift: float32 [1024], P('tp'), may hold values from -3 to 3
- out_weight: bfloat16 [1024, 2048], P('tp'), may hold values from -0.1875 to 0.1875
- residual: bfloat16 [4096, 2048], P('sp', 'tp'), may hold values from -10 to 10
- mix_gain: float32 [2048], P('tp'), may hold values from 0.1 to 1.9
- expert_ids: int32 [4096, 2], P('sp'), may hold values from 0 to 7, all different within a row; in each aligned block of 128 rows (0 to 127, 128 to 255, ...) at most 64 rows name the same one
- group_weight: float32 [4096], P('sp'), may hold values from 0.6 to 1
- score_gap: float32 [4096], P('sp'), may hold values from -0.8 to 0.8
- w_gate: bfloat16 [8, 2048, 1024], P('sp', None, 'tp'), may hold values from -0.125 to 0.125
- w_up: bfloat16 [8, 2048, 1024], P('sp', None, 'tp'), may hold values from -0.125 to 0.125
- w_down: bfloat16 [8, 1024, 2048], P('sp', 'tp'), may hold values from -0.1875 to 0.1875
Outputs:
- layer_out: bfloat16 [4096, 2048], P('sp', 'tp')
The draws below stay inside these ranges and needn't reach their ends.
Inputs may be any that keep to these rules, and one draw needn't show every extreme that they name: `expert_ids`: the two experts of a position differ. In each aligned block of 512 // 4 positions no expert is named by more than 64 rows, a bound that some block reaches.
All inputs are finite; a program needn't handle non-finite values.
Results may differ from the reference program's by a relative error of at most 0.012.
Values may be sent and summed in bfloat16 or wider, within the bound.
A program may use at most 128 MiB of HBM per device.

```python
import math
import jax
import jax.numpy as jnp
import numpy as np
from jax import lax

D = 2048
CH = 1024
FF = 1024
KW = 31
ROWS = 512
TOKENS = 4096
EXPERTS = 8
CAP = 64
N_SP = 8
N_TP = 4


def draw_conv_weight(key, part):
    rising = jnp.exp(jnp.linspace(math.log(0.3), math.log(3.0), CH)).astype(jnp.float32)
    base = jnp.clip(jax.random.normal(key, (KW, CH), jnp.float32), -4.0, 4.0)
    return (base * rising[None, :] / math.sqrt(KW)).astype(jnp.float32)


def draw_residual(key, part):
    rising = jnp.exp(jnp.linspace(math.log(0.5), math.log(2.0), D)).astype(jnp.float32)
    base = jnp.clip(jax.random.normal(key, (TOKENS, D), jnp.float32), -5.0, 5.0)
    return (base * rising[None, :]).astype(jnp.bfloat16)


def levels(key, extent, shards, smallest, high):
    def one(axis_at, blocks):
        steps = jax.random.uniform(jax.random.fold_in(jax.random.fold_in(key, 6), axis_at), (blocks,), jnp.float32, smallest / len(shards), high / len(shards))
        return jnp.repeat(jnp.exp(steps), extent[axis_at] // blocks).reshape((-1,) + (1,) * (len(extent) - axis_at - 1))

    level = one(*shards[0])
    for cut in shards[1:]:
        level = level * one(*cut)
    return level


def assign_block(stream_key, own, number, rows, amount, top, bound, lean):
    sequence = jax.random.permutation(stream_key, amount)
    heavy_load, common = load_shares(amount, rows * top, bound, lean, True), load_shares(amount, rows * top, bound, lean, False)
    places = jnp.arange(amount)

    def named(tallies, offset_by):
        used = int((tallies > 0).sum())
        fixed = max(1, used // 4)
        passed = fixed + (places - fixed + offset_by * (used - fixed)) % max(1, amount - fixed)
        return jnp.zeros((amount,), jnp.int32).at[sequence[jnp.where(places < fixed, places, passed)]].set(jnp.asarray(tallies, jnp.int32))

    tallies = jnp.where(number % 4 == 0, named(heavy_load, number // 4), named(common, number - number // 4 - 1))
    mixed = jax.random.permutation(jax.random.fold_in(own, 3), amount)
    donor, receiver = mixed[0:amount // 2 * 2:2], mixed[1:amount // 2 * 2:2]
    margin = jnp.minimum(tallies[donor] - 1, bound - tallies[receiver]) // 2
    margin = jnp.where((donor == sequence[0]) | (receiver == sequence[0]) | (tallies[receiver] == 0), 0, jnp.maximum(margin, 0))
    passed = jax.random.randint(jax.random.fold_in(own, 4), (amount // 2,), 0, 1 << 20) % (margin + 1)
    tallies = tallies.at[donor].add(-passed).at[receiver].add(passed)
    items = jnp.searchsorted(jnp.cumsum(tallies), jnp.arange(rows * top), side="right").astype(jnp.int32)
    grid = items.reshape(top, rows).T
    grid = grid[jax.random.permutation(jax.random.fold_in(own, 1), rows)]
    offset_by = jax.random.randint(jax.random.fold_in(own, 2), (rows, 1), 0, top)
    return jnp.take_along_axis(grid, (jnp.arange(top)[None, :] + offset_by) % top, axis=1)


def load_shares(count, total, most, skew, full):
    loads = [(1 << 20) // math.isqrt(standing ** skew) + 1 for standing in range(1, count + 1)]
    largest = most if full else min(most, max(-(-total // count), total * loads[0] // sum(loads)))
    least = 1 if total - largest >= count - 1 else 0
    holding, surplus = [largest] + [least] * (count - 1), total - largest - least * (count - 1)
    while surplus > 0:
        candidates = [i for i in range(1, count) if holding[i] < largest] or [i for i in range(1, count) if holding[i] < most]
        pool, left = sum([loads[i] for i in candidates]), surplus
        for i in candidates:
            extra = min(most - holding[i], max(1, left * loads[i] // pool), surplus)
            holding[i] = holding[i] + extra
            surplus = surplus - extra
    return np.array(holding)


def scatter_about(own_key, shape, spread, reach, split=(), kind=jnp.bfloat16):
    entries = jax.random.normal(own_key, shape, jnp.float32) * spread
    if len(split) > 0:
        entries = levels(own_key, shape, split, -0.22, 0.18) * entries
    return jnp.clip(entries, min=-reach, max=reach).astype(kind)


def setup_inputs(seed: int = 0) -> dict:
    splits = jax.random.split(jax.random.key(seed), 15)
    conv_value = scatter_about(splits[0], (TOKENS, CH), 1.0, 6.0, ((0, 8), (1, 4)))
    conv_gate = scatter_about(splits[1], (TOKENS, CH), 1.5, 9.0, ((0, 8), (1, 4)))
    conv_weight = draw_conv_weight(jax.random.fold_in(splits[14], 71), 0)
    conv_gain = jnp.clip(1.0 + 0.18 * jax.random.normal(splits[3], (CH,), jnp.float32), 0.1, 1.9)
    conv_shift = scatter_about(splits[4], (CH,), 0.5, 3.0, ((0, 4),), jnp.float32)
    out_weight = scatter_about(splits[5], (CH, D), CH ** -0.5, 0.1875, ((0, 4),))
    residual = draw_residual(jax.random.fold_in(splits[14], 71), 0)
    mix_gain = jnp.clip(1.0 + 0.18 * jax.random.normal(splits[7], (D,), jnp.float32), 0.1, 1.9)
    expert_ids_keys = jax.random.split(jax.random.fold_in(splits[8], 1), TOKENS // (ROWS // N_TP))
    expert_ids_turns = jax.random.permutation(jax.random.fold_in(splits[8], 3), TOKENS // (ROWS // N_TP))
    expert_ids = jax.vmap(lambda own, number: assign_block(jax.random.fold_in(splits[8], 2), own, number, ROWS // N_TP, EXPERTS, 2, CAP, 2))(expert_ids_keys, expert_ids_turns).reshape((TOKENS, 2))
    group_weight = jnp.clip(0.6 + 0.39999998 * jax.random.uniform(splits[9], (TOKENS,), jnp.float32) ** levels(splits[9], (TOKENS,), ((0, 8),), -0.2, 0.2), 0.6, 1.0)
    score_gap = jnp.clip(jax.random.uniform(splits[10], (TOKENS,), jnp.float32, -0.8, 0.8) * levels(splits[10], (TOKENS,), ((0, 8),), -0.4, 0.0), -0.8, 0.8)
    w_gate = scatter_about(splits[11], (EXPERTS, D, FF), D ** -0.5, 0.125, ((0, 8), (2, 4)))
    w_up = scatter_about(splits[12], (EXPERTS, D, FF), D ** -0.5, 0.125, ((0, 8), (2, 4)))
    w_down = scatter_about(splits[13], (EXPERTS, FF, D), FF ** -0.5, 0.1875, ((0, 8), (1, 4)))
    return {"conv_value": conv_value, "conv_gate": conv_gate, "conv_weight": conv_weight, "conv_gain": conv_gain, "conv_shift": conv_shift, "out_weight": out_weight, "residual": residual, "mix_gain": mix_gain, "expert_ids": expert_ids, "group_weight": group_weight, "score_gap": score_gap, "w_gate": w_gate, "w_up": w_up, "w_down": w_down}


eps = 1e-06

def reference(conv_value, conv_gate, conv_weight, conv_gain, conv_shift, out_weight, residual, mix_gain, expert_ids, group_weight, score_gap, w_gate, w_up, w_down):
    gated = conv_value.astype(jnp.float32) * jax.nn.sigmoid(conv_gate.astype(jnp.float32))
    padded = jnp.pad(gated, ((KW - 1, 0), (0, 0)))
    convolved = jnp.zeros_like(gated)
    for tap_index in range(KW):
        convolved = convolved + conv_weight[tap_index] * padded[tap_index:tap_index + TOKENS]
    row_mean = lax.optimization_barrier(jnp.mean(convolved, axis=-1, keepdims=True))
    row_var = lax.optimization_barrier(jnp.mean(convolved * convolved, axis=-1, keepdims=True)) - row_mean * row_mean
    normalized = (convolved - row_mean) * lax.rsqrt(row_var + eps) * conv_gain + conv_shift
    activated = jax.nn.silu(normalized).astype(jnp.bfloat16)
    block_width = CH // N_TP
    mixed = jnp.zeros((TOKENS, D), jnp.float32)
    for block_index in range(N_TP):
        low = block_index * block_width
        term = jnp.dot(activated[:, low:low + block_width], out_weight[low:low + block_width], preferred_element_type=jnp.float32)
        mixed = mixed + term.astype(jnp.bfloat16).astype(jnp.float32)
    middle = (residual.astype(jnp.float32) + mixed).astype(jnp.bfloat16)
    middle_wide = middle.astype(jnp.float32)
    normed = (middle_wide * lax.rsqrt(lax.optimization_barrier(jnp.mean(middle_wide * middle_wide, axis=-1, keepdims=True)) + eps) * mix_gain).astype(jnp.bfloat16)
    assign_count = TOKENS * 2
    expert_cap = N_SP * N_TP * CAP
    flat_experts = expert_ids.reshape(-1)
    token_of = jnp.concatenate([jnp.arange(assign_count, dtype=jnp.int32) // 2, jnp.array([TOKENS], jnp.int32)])
    normed_pad = jnp.concatenate([normed, jnp.zeros((1, D), jnp.bfloat16)], axis=0).astype(jnp.float32)
    hidden_width = FF // N_TP

    def expert_step(carry, expert):
        positions = jnp.nonzero(flat_experts == expert, size=expert_cap, fill_value=assign_count)[0].astype(jnp.int32)
        chosen = normed_pad[token_of[positions]]
        gate_part = jnp.dot(chosen, w_gate[expert].astype(jnp.float32))
        up_part = jnp.dot(chosen, w_up[expert].astype(jnp.float32))
        hidden = (jax.nn.silu(gate_part) * up_part).astype(jnp.bfloat16).astype(jnp.float32)
        down = w_down[expert].astype(jnp.float32)
        total = jnp.zeros((expert_cap, D), jnp.float32)
        for block_index in range(N_TP):
            low = block_index * hidden_width
            term = jnp.dot(hidden[:, low:low + hidden_width], down[low:low + hidden_width])
            total = total + term.astype(jnp.bfloat16).astype(jnp.float32)
        carry = carry.at[positions].set(total.astype(jnp.bfloat16))
        return (carry, None)
    start = jnp.zeros((assign_count + 1, D), jnp.bfloat16)
    results, _ = lax.scan(expert_step, start, jnp.arange(EXPERTS, dtype=jnp.int32))
    picked = results[:assign_count].reshape(TOKENS, 2, D).astype(jnp.float32)
    first_gate = group_weight * jax.nn.sigmoid(score_gap)
    second_gate = group_weight * jax.nn.sigmoid(-score_gap)
    layer_out = middle_wide + first_gate[:, None] * picked[:, 0] + second_gate[:, None] * picked[:, 1]
    return layer_out.astype(jnp.bfloat16)
```

```python
import functools
import jax
import jax.numpy as jnp
from jax import lax
from jax.experimental import pallas as pl
from jax.experimental.pallas import tpu as pltpu
from jax.sharding import PartitionSpec as P

eps = 1e-06


def passed_along(value, axis, steps):
    count = lax.axis_size(axis)
    leading, last = (max(0, -steps), min(count, count - steps))
    return lax.ppermute(value, axis, [(source, source + steps) for source in range(leading, last)])


def sigmoid(v):
    return 1.0 / (1.0 + jnp.exp(-v))


def mix_kernel(rows, conv_ref, res_ref, weight_ref, slots_ref, middle_ref, out_ref):
    blocks, _, width = conv_ref.shape
    channels = blocks * width
    columns = res_ref.shape[2]
    features = blocks * columns
    total = jnp.zeros((rows, 1), jnp.float32)
    squares = jnp.zeros((rows, 1), jnp.float32)
    for b in range(blocks):
        part = conv_ref[b, :rows, :]
        total = total + jnp.sum(part, axis=-1, keepdims=True)
        squares = squares + jnp.sum(part * part, axis=-1, keepdims=True)
    mean = total / channels
    scale = lax.rsqrt(squares / channels - mean * mean + eps)
    mixed = jnp.zeros((rows, features), jnp.float32)
    for b in range(blocks):
        gain = conv_ref[b, rows : rows + 1, :]
        shift = conv_ref[b, rows + 1 : rows + 2, :]
        normalized = (conv_ref[b, :rows, :] - mean) * scale * gain + shift
        activated = (normalized * sigmoid(normalized)).astype(jnp.bfloat16)
        term = jnp.dot(activated, weight_ref[b], preferred_element_type=jnp.float32)
        mixed = mixed + term
    row_sq = jnp.zeros((rows, 1), jnp.float32)
    for b in range(blocks):
        span = slice(b * columns, (b + 1) * columns)
        middle = (res_ref[b].astype(jnp.float32) + mixed[:, span]).astype(jnp.bfloat16)
        middle_ref[b] = middle
        wide = middle.astype(jnp.float32)
        row_sq = row_sq + jnp.sum(wide * wide, axis=-1, keepdims=True)
    scale = lax.rsqrt(row_sq / features + eps)
    slot_num = out_ref.shape[0]
    at = lax.broadcasted_iota(jnp.int32, (slot_num, rows), 0)
    place = jnp.where((at == slots_ref[0:1, :]) | (at == slots_ref[1:2, :]), 1.0, 0.0).astype(jnp.bfloat16)
    pieces = columns // width
    for b in range(blocks):
        gains = [conv_ref[b, rows + 2 + i : rows + 3 + i, :] for i in range(pieces)]
        for i in range(pieces):
            wide = middle_ref[b, :, i * width : (i + 1) * width].astype(jnp.float32)
            normed = (wide * scale * gains[i]).astype(jnp.bfloat16)
            low = b * columns + i * width
            out_ref[:, low : low + width] = jnp.dot(
                place, normed, preferred_element_type=jnp.float32
            ).astype(jnp.bfloat16)


def mix(conv, residual, weight, slots, slot_num):
    blocks, rows, columns = residual.shape
    return pl.pallas_call(
        functools.partial(mix_kernel, rows),
        out_shape=(
            jax.ShapeDtypeStruct(residual.shape, jnp.bfloat16),
            jax.ShapeDtypeStruct((slot_num, blocks * columns), jnp.bfloat16),
        ),
        in_specs=[pl.BlockSpec(memory_space=pltpu.VMEM)] * 4,
        out_specs=[pl.BlockSpec(memory_space=pltpu.VMEM)] * 2,
        cost_estimate=pl.CostEstimate(
            flops=2 * rows * weight.size + 2 * slot_num * rows * blocks * columns,
            bytes_accessed=2 * weight.size + 4 * conv.size,
            transcendentals=0,
        ),
    )(conv, residual, weight, slots)


def expert_kernel(x_ref, gate_ref, up_ref, down_ref, out_ref, total):
    step = pl.program_id(0)

    @pl.when(step == 0)
    def _():
        total[...] = jnp.zeros_like(total)

    x = x_ref[...]
    gate = jnp.dot(x, gate_ref[0], preferred_element_type=jnp.float32)
    up = jnp.dot(x, up_ref[0], preferred_element_type=jnp.float32)
    hidden = (gate * sigmoid(gate) * up).astype(jnp.bfloat16)
    total[...] += jnp.dot(hidden, down_ref[0], preferred_element_type=jnp.float32)

    @pl.when(step == pl.num_programs(0) - 1)
    def _():
        out_ref[...] = total[...].astype(jnp.bfloat16)


def expert(x, w_gate, w_up, w_down):
    rows, features = x.shape
    blocks, _, width = w_gate.shape
    return pl.pallas_call(
        expert_kernel,
        grid=(blocks,),
        out_shape=jax.ShapeDtypeStruct((rows, features), jnp.bfloat16),
        in_specs=[
            pl.BlockSpec((rows, features), lambda b: (0, 0)),
            pl.BlockSpec((1, features, width), lambda b: (b, 0, 0)),
            pl.BlockSpec((1, features, width), lambda b: (b, 0, 0)),
            pl.BlockSpec((1, width, features), lambda b: (b, 0, 0)),
        ],
        out_specs=pl.BlockSpec((rows, features), lambda b: (0, 0)),
        scratch_shapes=[pltpu.VMEM((rows, features), jnp.float32)],
        cost_estimate=pl.CostEstimate(
            flops=6 * rows * w_gate.size,
            bytes_accessed=6 * w_gate.size + 4 * rows * features,
            transcendentals=rows * blocks * width,
        ),
    )(x, w_gate, w_up, w_down)


def combine_kernel(back_ref, middle_ref, slots_ref, gates_ref, out_ref):
    blocks, rows, columns = middle_ref.shape
    slot_num = back_ref.shape[0]
    at = lax.broadcasted_iota(jnp.int32, (rows, slot_num), 1)
    picks = [
        jnp.where(at == slots_ref[:, k : k + 1], 1.0, 0.0).astype(jnp.bfloat16) for k in range(2)
    ]
    weight, gap = gates_ref[:, 0:1], gates_ref[:, 1:2]
    gates = [weight * sigmoid(gap), weight * sigmoid(-gap)]
    for b in range(blocks):
        part = back_ref[:, b * columns : (b + 1) * columns]
        total = middle_ref[b].astype(jnp.float32)
        for k in range(2):
            total = total + gates[k] * jnp.dot(picks[k], part, preferred_element_type=jnp.float32)
        out_ref[b] = total.astype(jnp.bfloat16)


def combine(back, middle, slots, gates):
    return pl.pallas_call(
        combine_kernel,
        out_shape=jax.ShapeDtypeStruct(middle.shape, jnp.bfloat16),
        in_specs=[pl.BlockSpec(memory_space=pltpu.VMEM)] * 4,
        out_specs=pl.BlockSpec(memory_space=pltpu.VMEM),
        cost_estimate=pl.CostEstimate(
            flops=4 * middle.size * back.shape[0], bytes_accessed=2 * back.size, transcendentals=0
        ),
    )(back, middle, slots, gates)


def shards(
    conv_value,
    conv_gate,
    conv_weight,
    conv_gain,
    conv_shift,
    out_weight,
    residual,
    mix_gain,
    expert_ids,
    group_weight,
    score_gap,
    w_gate,
    w_up,
    w_down,
):
    row_count, width = conv_value.shape
    columns = residual.shape[1]
    reach_rows = conv_weight.shape[0] - 1
    seq_devices = lax.axis_size("sp")
    tp_devices = lax.axis_size("tp")
    quarter = row_count // tp_devices
    capacity = 4 * quarter // seq_devices
    slot_num = seq_devices * capacity
    my_index = lax.axis_index("tp")

    out_all = lax.all_gather(out_weight, "tp", axis=0, tiled=False)
    w_gate, w_up, w_down, _ = lax.optimization_barrier((w_gate[0], w_up[0], w_down[0], out_weight))
    gate_all = lax.all_gather(w_gate, "tp", axis=0, tiled=False)
    up_all = lax.all_gather(w_up, "tp", axis=0, tiled=False)
    down_all = lax.all_gather(w_down, "tp", axis=0, tiled=False)

    tails = jnp.concatenate(
        [conv_value[row_count - reach_rows :], conv_gate[row_count - reach_rows :]], axis=1
    )
    previous = passed_along(tails, "sp", 1)
    res_rows = lax.all_to_all(
        residual.reshape(tp_devices, quarter, columns), "tp", split_axis=0, concat_axis=0, tiled=True
    )
    values = jnp.concatenate([previous[:, :width], conv_value], axis=0).astype(jnp.float32)
    gate_pre = jnp.concatenate([previous[:, width:], conv_gate], axis=0).astype(jnp.float32)
    gated = values * jax.nn.sigmoid(gate_pre)
    convolved = jnp.zeros((row_count, width), jnp.float32)
    for tap_index in range(reach_rows + 1):
        convolved = convolved + conv_weight[tap_index] * gated[tap_index : tap_index + row_count]
    extras = jnp.concatenate(
        [conv_gain[None], conv_shift[None], mix_gain.reshape(-1, width)], axis=0
    )
    extras = jnp.pad(extras, ((0, -extras.shape[0] % 8), (0, 0)))
    message = jnp.concatenate(
        [
            convolved.reshape(tp_devices, quarter, width),
            jnp.broadcast_to(extras[None], (tp_devices,) + extras.shape),
        ],
        axis=1,
    )
    conv_rows = lax.all_to_all(message, "tp", split_axis=0, concat_axis=0, tiled=True)

    own = lax.dynamic_slice_in_dim(expert_ids, my_index * quarter, quarter, 0)
    flat = own.reshape(-1)
    onehot = (flat[:, None] == jnp.arange(seq_devices, dtype=jnp.int32)[None, :]).astype(jnp.bfloat16)
    order = jnp.arange(quarter * 2)
    lower = (order[:, None] > order[None, :]).astype(jnp.bfloat16)
    before = jnp.dot(lower, onehot, preferred_element_type=jnp.float32)
    rank = jnp.sum(before * onehot.astype(jnp.float32), axis=-1).astype(jnp.int32)
    slots = (flat * capacity + rank).reshape(quarter, 2)

    middle, outgoing = mix(conv_rows, res_rows, out_all, slots.T, slot_num)
    received = lax.all_to_all(
        outgoing.reshape(seq_devices, capacity, -1), "sp", split_axis=0, concat_axis=0, tiled=True
    )
    outputs = expert(received.reshape(slot_num, -1), gate_all, up_all, down_all)
    returned = lax.all_to_all(
        outputs.reshape(seq_devices, capacity, -1), "sp", split_axis=0, concat_axis=0, tiled=True
    )
    gates = jnp.stack([group_weight, score_gap], axis=1)
    own_gates = lax.dynamic_slice_in_dim(gates, my_index * quarter, quarter, 0)
    result = combine(returned.reshape(slot_num, -1), middle, slots, own_gates)
    result = lax.all_to_all(result, "tp", split_axis=0, concat_axis=0, tiled=True)
    return result.reshape(row_count, columns)


def solution(mesh):
    return jax.shard_map(
        shards,
        mesh=mesh,
        in_specs=(
            P("sp", "tp"),
            P("sp", "tp"),
            P(None, "tp"),
            P("tp"),
            P("tp"),
            P("tp", None),
            P("sp", "tp"),
            P("tp"),
            P("sp", None),
            P("sp"),
            P("sp"),
            P("sp", None, "tp"),
            P("sp", None, "tp"),
            P("sp", "tp", None),
        ),
        out_specs=P("sp", "tp"),
        check_vma=False,
    )
```

```python
import functools
import jax
import jax.numpy as jnp
from jax import lax
from jax.experimental import pallas as pl
from jax.experimental.pallas import tpu as pltpu
from jax.sharding import PartitionSpec as P

eps = 1e-06


def passed_along(value, axis, steps):
    count = lax.axis_size(axis)
    leading, last = (max(0, -steps), min(count, count - steps))
    return lax.ppermute(value, axis, [(source, source + steps) for source in range(leading, last)])


def sigmoid(v):
    return 1.0 / (1.0 + jnp.exp(-v))


def mix_kernel(rows, conv_ref, res_ref, weight_ref, slots_ref, middle_ref, out_ref):
    blocks, _, width = conv_ref.shape
    channels = blocks * width
    columns = res_ref.shape[2]
    features = blocks * columns
    total = jnp.zeros((rows, 1), jnp.float32)
    squares = jnp.zeros((rows, 1), jnp.float32)
    for b in range(blocks):
        part = conv_ref[b, :rows, :]
        total = total + jnp.sum(part, axis=-1, keepdims=True)
        squares = squares + jnp.sum(part * part, axis=-1, keepdims=True)
    mean = total / channels
    scale = lax.rsqrt(squares / channels - mean * mean + eps)
    mixed = jnp.zeros((rows, features), jnp.float32)
    for b in range(blocks):
        gain = conv_ref[b, rows : rows + 1, :]
        shift = conv_ref[b, rows + 1 : rows + 2, :]
        normalized = (conv_ref[b, :rows, :] - mean) * scale * gain + shift
        activated = (normalized * sigmoid(normalized)).astype(jnp.bfloat16)
        term = jnp.dot(activated, weight_ref[b], preferred_element_type=jnp.float32)
        mixed = mixed + term
    row_sq = jnp.zeros((rows, 1), jnp.float32)
    for b in range(blocks):
        span = slice(b * columns, (b + 1) * columns)
        middle = (res_ref[b].astype(jnp.float32) + mixed[:, span]).astype(jnp.bfloat16)
        middle_ref[b] = middle
        wide = middle.astype(jnp.float32)
        row_sq = row_sq + jnp.sum(wide * wide, axis=-1, keepdims=True)
    scale = lax.rsqrt(row_sq / features + eps)
    slot_num = out_ref.shape[0]
    at = lax.broadcasted_iota(jnp.int32, (slot_num, rows), 0)
    place = jnp.where((at == slots_ref[0:1, :]) | (at == slots_ref[1:2, :]), 1.0, 0.0).astype(jnp.bfloat16)
    pieces = columns // width
    for b in range(blocks):
        gains = [conv_ref[b, rows + 2 + i : rows + 3 + i, :] for i in range(pieces)]
        for i in range(pieces):
            wide = middle_ref[b, :, i * width : (i + 1) * width].astype(jnp.float32)
            normed = (wide * scale * gains[i]).astype(jnp.bfloat16)
            low = b * columns + i * width
            out_ref[:, low : low + width] = jnp.dot(
                place, normed, preferred_element_type=jnp.float32
            ).astype(jnp.bfloat16)


def mix(conv, residual, weight, slots, slot_num):
    blocks, rows, columns = residual.shape
    return pl.pallas_call(
        functools.partial(mix_kernel, rows),
        out_shape=(
            jax.ShapeDtypeStruct(residual.shape, jnp.bfloat16),
            jax.ShapeDtypeStruct((slot_num, blocks * columns), jnp.bfloat16),
        ),
        in_specs=[pl.BlockSpec(memory_space=pltpu.VMEM)] * 4,
        out_specs=[pl.BlockSpec(memory_space=pltpu.VMEM)] * 2,
        cost_estimate=pl.CostEstimate(
            flops=2 * rows * weight.size + 2 * slot_num * rows * blocks * columns,
            bytes_accessed=2 * weight.size + 4 * conv.size,
            transcendentals=0,
        ),
    )(conv, residual, weight, slots)


def expert_kernel(
    seq_num,
    x_ref,
    gate_ref,
    up_ref,
    down_ref,
    middle_ref,
    slots_ref,
    gates_ref,
    out_ref,
    received,
    gate_all,
    up_all,
    down_all,
    total,
    outputs,
    back,
    result,
    final,
    x_send,
    x_recv,
    w_send,
    w_recv,
    y_send,
    y_recv,
    r_send,
    r_recv,
    own_sem,
):
    blocks, rows, columns = middle_ref.shape
    slot_num = x_ref.shape[0]
    capacity = slot_num // seq_num
    me, mine = lax.axis_index("sp"), lax.axis_index("tp")
    partner = mine + 1 - 2 * lax.rem(mine, 2)
    counter = lax.rem(mine + blocks // 2, blocks)
    diagonal = lax.rem(partner + blocks // 2, blocks)
    mates = (partner, counter, diagonal)
    steps = sorted(range(1, seq_num), key=lambda i: abs(2 * i - seq_num))

    def to_seq(i):
        return {"sp": lax.rem(me + i, seq_num)}

    barrier = pltpu.get_barrier_semaphore()
    for mate in mates:
        pl.semaphore_signal(barrier, inc=1, device_id={"tp": mate}, device_id_type=pl.DeviceIdType.MESH)
    for i in steps:
        pl.semaphore_signal(barrier, inc=1, device_id=to_seq(i), device_id_type=pl.DeviceIdType.MESH)
    pl.semaphore_wait(barrier, len(mates) + len(steps))

    def remote(src, dst, send, recv, device):
        copy = pltpu.make_async_remote_copy(
            src_ref=src,
            dst_ref=dst,
            send_sem=send,
            recv_sem=recv,
            device_id=device,
            device_id_type=pl.DeviceIdType.MESH,
        )
        copy.start()
        return copy

    def at(index):
        return pl.ds(pl.multiple_of(index * capacity, capacity), capacity)

    weights = ((gate_ref, gate_all), (up_ref, up_all), (down_ref, down_all))
    across, beside, own = [], [], []
    for k, (source, held) in enumerate(weights):
        across.append(
            remote(source, held.at[2], w_send.at[k, 2], w_recv.at[k, 2], {"tp": counter})
        )
    x_copies = []
    for i in steps:
        peer = lax.rem(me + i, seq_num)
        x_copies.append(
            remote(x_ref.at[at(peer)], received.at[at(me)], x_send.at[i], x_recv.at[i], to_seq(i))
        )
    for k, (source, held) in enumerate(weights):
        beside.append(
            remote(source, held.at[1], w_send.at[k, 1], w_recv.at[k, 1], {"tp": partner})
        )
        copy = pltpu.make_async_copy(source, held.at[0], own_sem.at[k])
        copy.start()
        own.append(copy)
    own_x = pltpu.make_async_copy(x_ref.at[at(me)], received.at[at(me)], own_sem.at[3])
    own_x.start()

    def forward(k):
        held = weights[k][1]
        across[k].wait_recv()
        return remote(held.at[2], held.at[3], w_send.at[k, 3], w_recv.at[k, 3], {"tp": partner})

    total[...] = jnp.zeros_like(total)
    passed = [forward(0), forward(1)]
    own_x.wait()
    for copy in own:
        copy.wait()
    for copy in beside:
        copy.wait_recv()
    for copy in x_copies:
        copy.wait_recv()
    passed_down = pltpu.make_async_remote_copy(
        src_ref=down_all.at[2],
        dst_ref=down_all.at[3],
        send_sem=w_send.at[2, 3],
        recv_sem=w_recv.at[2, 3],
        device_id={"tp": partner},
        device_id_type=pl.DeviceIdType.MESH,
    )

    @pl.loop(0, blocks)
    def _(b):
        @pl.when(b == 2)
        def _():
            across[2].wait_recv()
            passed_down.start()

        @pl.when(b == 3)
        def _():
            for copy in passed:
                copy.wait_recv()
            passed_down.wait_recv()

        x = received[...]
        gate = jnp.dot(x, gate_all[b], preferred_element_type=jnp.float32)
        up = jnp.dot(x, up_all[b], preferred_element_type=jnp.float32)
        hidden = (gate * sigmoid(gate) * up).astype(jnp.bfloat16)
        total[...] += jnp.dot(hidden, down_all[b], preferred_element_type=jnp.float32)

    outputs[...] = total[...].astype(jnp.bfloat16)
    y_copies = []
    for i in steps:
        peer = lax.rem(me + i, seq_num)
        y_copies.append(
            remote(outputs.at[at(peer)], back.at[at(me)], y_send.at[i], y_recv.at[i], to_seq(i))
        )
    own_y = pltpu.make_async_copy(outputs.at[at(me)], back.at[at(me)], own_sem.at[4])
    own_y.start()
    for copy in across + beside + passed + [passed_down] + x_copies:
        copy.wait_send()
    where = lax.broadcasted_iota(jnp.int32, (rows, slot_num), 1)
    picks = [
        jnp.where(where == slots_ref[:, k : k + 1], 1.0, 0.0).astype(jnp.bfloat16) for k in range(2)
    ]
    weight, gap = gates_ref[:, 0:1], gates_ref[:, 1:2]
    gates = [weight * sigmoid(gap), weight * sigmoid(-gap)]
    own_y.wait()
    for copy in y_copies:
        copy.wait_recv()
    for b in range(blocks):
        part = back[:, b * columns : (b + 1) * columns]
        value = middle_ref[b].astype(jnp.float32)
        for k in range(2):
            value = value + gates[k] * jnp.dot(picks[k], part, preferred_element_type=jnp.float32)
        result[b] = value.astype(jnp.bfloat16)
    rows_at = pl.ds(pl.multiple_of(mine * rows, rows), rows)
    r_copies = []
    for j, mate in ((1, counter), (2, diagonal), (0, partner)):
        r_copies.append(
            remote(result.at[mate], final.at[rows_at], r_send.at[j], r_recv.at[j], {"tp": mate})
        )
    own_r = pltpu.make_async_copy(result.at[mine], final.at[rows_at], own_sem.at[5])
    own_r.start()
    for copy in y_copies:
        copy.wait_send()
    own_r.wait()
    for copy in r_copies:
        copy.wait()
    out_ref[...] = final[...]


def expert(x, w_gate, w_up, w_down, middle, slots, gates, seq_num):
    slot_num, features = x.shape
    blocks, rows, columns = middle.shape
    width = w_gate.shape[1]
    vmem, anywhere = pl.BlockSpec(memory_space=pltpu.VMEM), pl.BlockSpec(memory_space=pl.ANY)
    wide = (slot_num, features)
    dma = pltpu.SemaphoreType.DMA
    return pl.pallas_call(
        functools.partial(expert_kernel, seq_num),
        out_shape=jax.ShapeDtypeStruct((blocks * rows, columns), jnp.bfloat16),
        in_specs=[vmem, anywhere, anywhere, anywhere, vmem, vmem, vmem],
        out_specs=vmem,
        scratch_shapes=[
            pltpu.VMEM(wide, jnp.bfloat16),
            pltpu.VMEM((blocks, features, width), jnp.bfloat16),
            pltpu.VMEM((blocks, features, width), jnp.bfloat16),
            pltpu.VMEM((blocks, width, features), jnp.bfloat16),
            pltpu.VMEM(wide, jnp.float32),
            pltpu.VMEM(wide, jnp.bfloat16),
            pltpu.VMEM(wide, jnp.bfloat16),
            pltpu.VMEM(middle.shape, jnp.bfloat16),
            pltpu.VMEM((blocks * rows, columns), jnp.bfloat16),
            dma((seq_num,)),
            dma((seq_num,)),
            dma((3, blocks)),
            dma((3, blocks)),
            dma((seq_num,)),
            dma((seq_num,)),
            dma((blocks,)),
            dma((blocks,)),
            dma((6,)),
        ],
        compiler_params=pltpu.CompilerParams(collective_id=0, has_side_effects=True),
        cost_estimate=pl.CostEstimate(
            flops=6 * slot_num * w_gate.size * blocks,
            bytes_accessed=6 * w_gate.size * blocks,
            transcendentals=slot_num * blocks * width,
        ),
    )(x, w_gate, w_up, w_down, middle, slots, gates)


def shards(
    conv_value,
    conv_gate,
    conv_weight,
    conv_gain,
    conv_shift,
    out_weight,
    residual,
    mix_gain,
    expert_ids,
    group_weight,
    score_gap,
    w_gate,
    w_up,
    w_down,
):
    row_count, width = conv_value.shape
    columns = residual.shape[1]
    reach_rows = conv_weight.shape[0] - 1
    seq_devices = lax.axis_size("sp")
    tp_devices = lax.axis_size("tp")
    quarter = row_count // tp_devices
    capacity = 4 * quarter // seq_devices
    slot_num = seq_devices * capacity
    my_index = lax.axis_index("tp")

    out_all = lax.all_gather(out_weight, "tp", axis=0, tiled=False)

    tails = jnp.concatenate(
        [conv_value[row_count - reach_rows :], conv_gate[row_count - reach_rows :]], axis=1
    )
    previous = passed_along(tails, "sp", 1)
    res_rows = lax.all_to_all(
        residual.reshape(tp_devices, quarter, columns), "tp", split_axis=0, concat_axis=0, tiled=True
    )
    values = jnp.concatenate([previous[:, :width], conv_value], axis=0).astype(jnp.float32)
    gate_pre = jnp.concatenate([previous[:, width:], conv_gate], axis=0).astype(jnp.float32)
    gated = values * jax.nn.sigmoid(gate_pre)
    convolved = jnp.zeros((row_count, width), jnp.float32)
    for tap_index in range(reach_rows + 1):
        convolved = convolved + conv_weight[tap_index] * gated[tap_index : tap_index + row_count]
    extras = jnp.concatenate(
        [conv_gain[None], conv_shift[None], mix_gain.reshape(-1, width)], axis=0
    )
    extras = jnp.pad(extras, ((0, -extras.shape[0] % 8), (0, 0)))
    message = jnp.concatenate(
        [
            convolved.reshape(tp_devices, quarter, width),
            jnp.broadcast_to(extras[None], (tp_devices,) + extras.shape),
        ],
        axis=1,
    )
    conv_rows = lax.all_to_all(message, "tp", split_axis=0, concat_axis=0, tiled=True)

    own = lax.dynamic_slice_in_dim(expert_ids, my_index * quarter, quarter, 0)
    flat = own.reshape(-1)
    onehot = (flat[:, None] == jnp.arange(seq_devices, dtype=jnp.int32)[None, :]).astype(jnp.bfloat16)
    order = jnp.arange(quarter * 2)
    lower = (order[:, None] > order[None, :]).astype(jnp.bfloat16)
    before = jnp.dot(lower, onehot, preferred_element_type=jnp.float32)
    rank = jnp.sum(before * onehot.astype(jnp.float32), axis=-1).astype(jnp.int32)
    slots = (flat * capacity + rank).reshape(quarter, 2)

    middle, outgoing = mix(conv_rows, res_rows, out_all, slots.T, slot_num)
    gates = jnp.stack([group_weight, score_gap], axis=1)
    own_gates = lax.dynamic_slice_in_dim(gates, my_index * quarter, quarter, 0)
    return expert(
        outgoing, w_gate[0], w_up[0], w_down[0], middle, slots, own_gates, seq_devices
    )


def solution(mesh):
    return jax.shard_map(
        shards,
        mesh=mesh,
        in_specs=(
            P("sp", "tp"),
            P("sp", "tp"),
            P(None, "tp"),
            P("tp"),
            P("tp"),
            P("tp", None),
            P("sp", "tp"),
            P("tp"),
            P("sp", None),
            P("sp"),
            P("sp"),
            P("sp", None, "tp"),
            P("sp", None, "tp"),
            P("sp", "tp", None),
        ),
        out_specs=P("sp", "tp"),
        check_vma=False,
    )
```

```python
import functools
import jax
import jax.numpy as jnp
from jax import lax
from jax.experimental import pallas as pl
from jax.experimental.pallas import tpu as pltpu
from jax.sharding import PartitionSpec as P

eps = 1e-06


def sigmoid(v):
    return 1.0 / (1.0 + jnp.exp(-v))


def mix_kernel(rows, conv_ref, res_ref, weight_ref, slots_ref, middle_ref, out_ref):
    blocks, _, width = conv_ref.shape
    channels = blocks * width
    columns = res_ref.shape[2]
    features = blocks * columns
    total = jnp.zeros((rows, 1), jnp.float32)
    squares = jnp.zeros((rows, 1), jnp.float32)
    for b in range(blocks):
        part = conv_ref[b, :rows, :]
        total = total + jnp.sum(part, axis=-1, keepdims=True)
        squares = squares + jnp.sum(part * part, axis=-1, keepdims=True)
    mean = total / channels
    scale = lax.rsqrt(squares / channels - mean * mean + eps)
    mixed = jnp.zeros((rows, features), jnp.float32)
    for b in range(blocks):
        gain = conv_ref[b, rows : rows + 1, :]
        shift = conv_ref[b, rows + 1 : rows + 2, :]
        normalized = (conv_ref[b, :rows, :] - mean) * scale * gain + shift
        activated = (normalized * sigmoid(normalized)).astype(jnp.bfloat16)
        term = jnp.dot(activated, weight_ref[b], preferred_element_type=jnp.float32)
        mixed = mixed + term
    row_sq = jnp.zeros((rows, 1), jnp.float32)
    for b in range(blocks):
        span = slice(b * columns, (b + 1) * columns)
        middle = (res_ref[b].astype(jnp.float32) + mixed[:, span]).astype(jnp.bfloat16)
        middle_ref[b] = middle
        wide = middle.astype(jnp.float32)
        row_sq = row_sq + jnp.sum(wide * wide, axis=-1, keepdims=True)
    scale = lax.rsqrt(row_sq / features + eps)
    slot_num = out_ref.shape[0]
    at = lax.broadcasted_iota(jnp.int32, (slot_num, rows), 0)
    place = jnp.where((at == slots_ref[0:1, :]) | (at == slots_ref[1:2, :]), 1.0, 0.0).astype(jnp.bfloat16)
    pieces = columns // width
    for b in range(blocks):
        gains = [conv_ref[b, rows + 2 + i : rows + 3 + i, :] for i in range(pieces)]
        for i in range(pieces):
            wide = middle_ref[b, :, i * width : (i + 1) * width].astype(jnp.float32)
            normed = (wide * scale * gains[i]).astype(jnp.bfloat16)
            low = b * columns + i * width
            out_ref[:, low : low + width] = jnp.dot(
                place, normed, preferred_element_type=jnp.float32
            ).astype(jnp.bfloat16)


def front_kernel(
    reach,
    value_ref,
    gate_ref,
    tap_ref,
    extra_ref,
    res_ref,
    weight_ref,
    slots_ref,
    middle_ref,
    out_ref,
    tail_value,
    tail_gate,
    gated,
    message,
    conv_rows,
    res_rows,
    weight_all,
    h_send,
    h_recv,
    w_send,
    w_recv,
    r_send,
    r_recv,
    c_send,
    c_recv,
    own_sem,
):
    blocks, rows, columns = res_ref.shape
    row_count = value_ref.shape[0]
    pad = tail_value.shape[0]
    me, mine = lax.axis_index("sp"), lax.axis_index("tp")
    seq_num = lax.axis_size("sp")
    partner = mine + 1 - 2 * lax.rem(mine, 2)
    counter = lax.rem(mine + blocks // 2, blocks)
    diagonal = lax.rem(partner + blocks // 2, blocks)
    after = {"sp": lax.rem(me + 1, seq_num)}
    before = {"sp": lax.rem(me + seq_num - 1, seq_num)}
    mates = ((1, counter), (2, diagonal), (0, partner))

    barrier = pltpu.get_barrier_semaphore()
    for device in [{"tp": mate} for _, mate in mates] + [before, after]:
        pl.semaphore_signal(barrier, inc=1, device_id=device, device_id_type=pl.DeviceIdType.MESH)
    pl.semaphore_wait(barrier, len(mates) + 2)

    def remote(src, dst, send, recv, device):
        copy = pltpu.make_async_remote_copy(
            src_ref=src,
            dst_ref=dst,
            send_sem=send,
            recv_sem=recv,
            device_id=device,
            device_id_type=pl.DeviceIdType.MESH,
        )
        copy.start()
        return copy

    last = pl.ds(row_count - pad, pad)
    halo = [
        remote(value_ref.at[last], tail_value, h_send.at[0], h_recv.at[0], after),
        remote(gate_ref.at[last], tail_gate, h_send.at[1], h_recv.at[1], after),
    ]
    res_copies = [
        remote(res_ref.at[mate], res_rows.at[mine], r_send.at[j], r_recv.at[j], {"tp": mate})
        for j, mate in mates
    ]
    across = remote(weight_ref, weight_all.at[mine], w_send.at[0], w_recv.at[0], {"tp": counter})
    beside = remote(weight_ref, weight_all.at[mine], w_send.at[1], w_recv.at[1], {"tp": partner})
    own = [
        pltpu.make_async_copy(weight_ref, weight_all.at[mine], own_sem.at[0]),
        pltpu.make_async_copy(res_ref.at[mine], res_rows.at[mine], own_sem.at[1]),
    ]
    for copy in own:
        copy.start()

    def gate_of(value, gate):
        return value.astype(jnp.float32) * sigmoid(gate.astype(jnp.float32))

    gated[pad:, :] = gate_of(value_ref[...], gate_ref[...])
    for copy in halo:
        copy.wait()
    first = gate_of(tail_value[...], tail_gate[...])
    gated[:pad, :] = jnp.where(me > 0, first, jnp.zeros_like(first))
    for b in range(blocks):
        for low in range(b * rows, (b + 1) * rows, rows // 2):
            part = jnp.zeros((rows // 2, value_ref.shape[1]), jnp.float32)
            for tap in range(reach + 1):
                begin = low + pad - reach + tap
                part = part + tap_ref[tap : tap + 1, :] * gated[begin : begin + rows // 2, :]
            message[b, low - b * rows : low - b * rows + rows // 2, :] = part
        message[b, rows:, :] = extra_ref[...]
    conv_copies = [
        remote(message.at[mate], conv_rows.at[mine], c_send.at[j], c_recv.at[j], {"tp": mate})
        for j, mate in mates
    ]
    own_conv = pltpu.make_async_copy(message.at[mine], conv_rows.at[mine], own_sem.at[2])
    own_conv.start()
    across.wait_recv()
    passed = remote(
        weight_all.at[counter], weight_all.at[counter], w_send.at[2], w_recv.at[2], {"tp": partner}
    )
    for copy in own + [own_conv]:
        copy.wait()
    for copy in res_copies + conv_copies + [beside, passed]:
        copy.wait()
    across.wait_send()
    mix_kernel(rows, conv_rows, res_rows, weight_all, slots_ref, middle_ref, out_ref)


def front(value, gate, taps, extras, residual, weight, slots, slot_num):
    blocks, rows, columns = residual.shape
    row_count, width = value.shape
    reach = taps.shape[0] - 1
    pad = reach + -reach % 16
    vmem, anywhere = pl.BlockSpec(memory_space=pltpu.VMEM), pl.BlockSpec(memory_space=pl.ANY)
    dma = pltpu.SemaphoreType.DMA
    sent = (blocks, rows + extras.shape[0], width)
    return pl.pallas_call(
        functools.partial(front_kernel, reach),
        out_shape=(
            jax.ShapeDtypeStruct(residual.shape, jnp.bfloat16),
            jax.ShapeDtypeStruct((slot_num, blocks * columns), jnp.bfloat16),
        ),
        in_specs=[vmem, vmem, vmem, vmem, vmem, anywhere, vmem],
        out_specs=[vmem, vmem],
        scratch_shapes=[
            pltpu.VMEM((pad, width), jnp.bfloat16),
            pltpu.VMEM((pad, width), jnp.bfloat16),
            pltpu.VMEM((pad + row_count, width), jnp.float32),
            pltpu.VMEM(sent, jnp.float32),
            pltpu.VMEM(sent, jnp.float32),
            pltpu.VMEM(residual.shape, jnp.bfloat16),
            pltpu.VMEM((blocks,) + weight.shape, jnp.bfloat16),
            dma((2,)),
            dma((2,)),
            dma((3,)),
            dma((3,)),
            dma((3,)),
            dma((3,)),
            dma((3,)),
            dma((3,)),
            dma((3,)),
        ],
        compiler_params=pltpu.CompilerParams(collective_id=1, has_side_effects=True),
        cost_estimate=pl.CostEstimate(
            flops=2 * rows * weight.size * blocks,
            bytes_accessed=8 * weight.size,
            transcendentals=0,
        ),
    )(value, gate, taps, extras, residual, weight, slots)


def expert_kernel(
    seq_num,
    x_ref,
    gate_ref,
    up_ref,
    down_ref,
    middle_ref,
    slots_ref,
    gates_ref,
    out_ref,
    received,
    gate_all,
    up_all,
    down_all,
    total,
    outputs,
    back,
    result,
    final,
    x_send,
    x_recv,
    w_send,
    w_recv,
    y_send,
    y_recv,
    r_send,
    r_recv,
    own_sem,
):
    blocks, rows, columns = middle_ref.shape
    slot_num = x_ref.shape[0]
    capacity = slot_num // seq_num
    me, mine = lax.axis_index("sp"), lax.axis_index("tp")
    partner = mine + 1 - 2 * lax.rem(mine, 2)
    counter = lax.rem(mine + blocks // 2, blocks)
    diagonal = lax.rem(partner + blocks // 2, blocks)
    mates = (partner, counter, diagonal)
    steps = sorted(range(1, seq_num), key=lambda i: abs(2 * i - seq_num))

    def to_seq(i):
        return {"sp": lax.rem(me + i, seq_num)}

    barrier = pltpu.get_barrier_semaphore()
    for mate in mates:
        pl.semaphore_signal(barrier, inc=1, device_id={"tp": mate}, device_id_type=pl.DeviceIdType.MESH)
    for i in steps:
        pl.semaphore_signal(barrier, inc=1, device_id=to_seq(i), device_id_type=pl.DeviceIdType.MESH)
    pl.semaphore_wait(barrier, len(mates) + len(steps))

    def remote(src, dst, send, recv, device):
        copy = pltpu.make_async_remote_copy(
            src_ref=src,
            dst_ref=dst,
            send_sem=send,
            recv_sem=recv,
            device_id=device,
            device_id_type=pl.DeviceIdType.MESH,
        )
        copy.start()
        return copy

    def at(index):
        return pl.ds(pl.multiple_of(index * capacity, capacity), capacity)

    weights = ((gate_ref, gate_all), (up_ref, up_all), (down_ref, down_all))
    across, beside, own = [], [], []
    for k, (source, held) in enumerate(weights):
        across.append(
            remote(source, held.at[2], w_send.at[k, 2], w_recv.at[k, 2], {"tp": counter})
        )
    x_copies = []
    for i in steps:
        peer = lax.rem(me + i, seq_num)
        x_copies.append(
            remote(x_ref.at[at(peer)], received.at[at(me)], x_send.at[i], x_recv.at[i], to_seq(i))
        )
    for k, (source, held) in enumerate(weights):
        beside.append(
            remote(source, held.at[1], w_send.at[k, 1], w_recv.at[k, 1], {"tp": partner})
        )
        copy = pltpu.make_async_copy(source, held.at[0], own_sem.at[k])
        copy.start()
        own.append(copy)
    own_x = pltpu.make_async_copy(x_ref.at[at(me)], received.at[at(me)], own_sem.at[3])
    own_x.start()

    def forward(k):
        held = weights[k][1]
        across[k].wait_recv()
        return remote(held.at[2], held.at[3], w_send.at[k, 3], w_recv.at[k, 3], {"tp": partner})

    total[...] = jnp.zeros_like(total)
    passed = [forward(0), forward(1)]
    own_x.wait()
    for copy in own:
        copy.wait()
    for copy in beside:
        copy.wait_recv()
    for copy in x_copies:
        copy.wait_recv()
    passed_down = pltpu.make_async_remote_copy(
        src_ref=down_all.at[2],
        dst_ref=down_all.at[3],
        send_sem=w_send.at[2, 3],
        recv_sem=w_recv.at[2, 3],
        device_id={"tp": partner},
        device_id_type=pl.DeviceIdType.MESH,
    )

    @pl.loop(0, blocks)
    def _(b):
        @pl.when(b == 2)
        def _():
            across[2].wait_recv()
            passed_down.start()

        @pl.when(b == 3)
        def _():
            for copy in passed:
                copy.wait_recv()
            passed_down.wait_recv()

        x = received[...]
        gate = jnp.dot(x, gate_all[b], preferred_element_type=jnp.float32)
        up = jnp.dot(x, up_all[b], preferred_element_type=jnp.float32)
        hidden = (gate * sigmoid(gate) * up).astype(jnp.bfloat16)
        total[...] += jnp.dot(hidden, down_all[b], preferred_element_type=jnp.float32)

    outputs[...] = total[...].astype(jnp.bfloat16)
    y_copies = []
    for i in steps:
        peer = lax.rem(me + i, seq_num)
        y_copies.append(
            remote(outputs.at[at(peer)], back.at[at(me)], y_send.at[i], y_recv.at[i], to_seq(i))
        )
    own_y = pltpu.make_async_copy(outputs.at[at(me)], back.at[at(me)], own_sem.at[4])
    own_y.start()
    for copy in across + beside + passed + [passed_down] + x_copies:
        copy.wait_send()
    where = lax.broadcasted_iota(jnp.int32, (rows, slot_num), 1)
    picks = [
        jnp.where(where == slots_ref[:, k : k + 1], 1.0, 0.0).astype(jnp.bfloat16) for k in range(2)
    ]
    weight, gap = gates_ref[:, 0:1], gates_ref[:, 1:2]
    gates = [weight * sigmoid(gap), weight * sigmoid(-gap)]
    own_y.wait()
    for copy in y_copies:
        copy.wait_recv()
    for b in range(blocks):
        part = back[:, b * columns : (b + 1) * columns]
        value = middle_ref[b].astype(jnp.float32)
        for k in range(2):
            value = value + gates[k] * jnp.dot(picks[k], part, preferred_element_type=jnp.float32)
        result[b] = value.astype(jnp.bfloat16)
    rows_at = pl.ds(pl.multiple_of(mine * rows, rows), rows)
    r_copies = []
    for j, mate in ((1, counter), (2, diagonal), (0, partner)):
        r_copies.append(
            remote(result.at[mate], final.at[rows_at], r_send.at[j], r_recv.at[j], {"tp": mate})
        )
    own_r = pltpu.make_async_copy(result.at[mine], final.at[rows_at], own_sem.at[5])
    own_r.start()
    for copy in y_copies:
        copy.wait_send()
    own_r.wait()
    for copy in r_copies:
        copy.wait()
    out_ref[...] = final[...]


def expert(x, w_gate, w_up, w_down, middle, slots, gates, seq_num):
    slot_num, features = x.shape
    blocks, rows, columns = middle.shape
    width = w_gate.shape[1]
    vmem, anywhere = pl.BlockSpec(memory_space=pltpu.VMEM), pl.BlockSpec(memory_space=pl.ANY)
    wide = (slot_num, features)
    dma = pltpu.SemaphoreType.DMA
    return pl.pallas_call(
        functools.partial(expert_kernel, seq_num),
        out_shape=jax.ShapeDtypeStruct((blocks * rows, columns), jnp.bfloat16),
        in_specs=[vmem, anywhere, anywhere, anywhere, vmem, vmem, vmem],
        out_specs=vmem,
        scratch_shapes=[
            pltpu.VMEM(wide, jnp.bfloat16),
            pltpu.VMEM((blocks, features, width), jnp.bfloat16),
            pltpu.VMEM((blocks, features, width), jnp.bfloat16),
            pltpu.VMEM((blocks, width, features), jnp.bfloat16),
            pltpu.VMEM(wide, jnp.float32),
            pltpu.VMEM(wide, jnp.bfloat16),
            pltpu.VMEM(wide, jnp.bfloat16),
            pltpu.VMEM(middle.shape, jnp.bfloat16),
            pltpu.VMEM((blocks * rows, columns), jnp.bfloat16),
            dma((seq_num,)),
            dma((seq_num,)),
            dma((3, blocks)),
            dma((3, blocks)),
            dma((seq_num,)),
            dma((seq_num,)),
            dma((blocks,)),
            dma((blocks,)),
            dma((6,)),
        ],
        compiler_params=pltpu.CompilerParams(collective_id=0, has_side_effects=True),
        cost_estimate=pl.CostEstimate(
            flops=6 * slot_num * w_gate.size * blocks,
            bytes_accessed=6 * w_gate.size * blocks,
            transcendentals=slot_num * blocks * width,
        ),
    )(x, w_gate, w_up, w_down, middle, slots, gates)


def shards(
    conv_value,
    conv_gate,
    conv_weight,
    conv_gain,
    conv_shift,
    out_weight,
    residual,
    mix_gain,
    expert_ids,
    group_weight,
    score_gap,
    w_gate,
    w_up,
    w_down,
):
    row_count, width = conv_value.shape
    columns = residual.shape[1]
    reach_rows = conv_weight.shape[0] - 1
    seq_devices = lax.axis_size("sp")
    tp_devices = lax.axis_size("tp")
    quarter = row_count // tp_devices
    capacity = 4 * quarter // seq_devices
    slot_num = seq_devices * capacity
    my_index = lax.axis_index("tp")

    extras = jnp.concatenate(
        [conv_gain[None], conv_shift[None], mix_gain.reshape(-1, width)], axis=0
    )
    extras = jnp.pad(extras, ((0, -extras.shape[0] % 8), (0, 0)))

    own = lax.dynamic_slice_in_dim(expert_ids, my_index * quarter, quarter, 0)
    flat = own.reshape(-1)
    onehot = (flat[:, None] == jnp.arange(seq_devices, dtype=jnp.int32)[None, :]).astype(jnp.bfloat16)
    order = jnp.arange(quarter * 2)
    lower = (order[:, None] > order[None, :]).astype(jnp.bfloat16)
    before = jnp.dot(lower, onehot, preferred_element_type=jnp.float32)
    rank = jnp.sum(before * onehot.astype(jnp.float32), axis=-1).astype(jnp.int32)
    slots = (flat * capacity + rank).reshape(quarter, 2)

    middle, outgoing = front(
        conv_value,
        conv_gate,
        conv_weight,
        extras,
        residual.reshape(tp_devices, quarter, columns),
        out_weight,
        slots.T,
        slot_num,
    )
    gates = jnp.stack([group_weight, score_gap], axis=1)
    own_gates = lax.dynamic_slice_in_dim(gates, my_index * quarter, quarter, 0)
    return expert(
        outgoing, w_gate[0], w_up[0], w_down[0], middle, slots, own_gates, seq_devices
    )


def solution(mesh):
    return jax.shard_map(
        shards,
        mesh=mesh,
        in_specs=(
            P("sp", "tp"),
            P("sp", "tp"),
            P(None, "tp"),
            P("tp"),
            P("tp"),
            P("tp", None),
            P("sp", "tp"),
            P("tp"),
            P("sp", None),
            P("sp"),
            P("sp"),
            P("sp", None, "tp"),
            P("sp", None, "tp"),
            P("sp", "tp", None),
        ),
        out_specs=P("sp", "tp"),
        check_vma=False,
    )
```
